32 devices in a mesh: sp: 8 (over z, y), tp: 4 (over x, core).
Axes of the slice: x: 2, y: 2, z: 4, core: 2. Of those that a mesh axis runs over, the one named last changes fastest.
Arguments:
- tokens: bfloat16 [8192, 2048], P('sp', 'tp'), may hold values from -6 to 6
- input_norm_gain: float32 [2048], replicated, may hold values from 0.1 to 1.9
- pooling_input_matrix: bfloat16 [2048, 512], P(None, 'tp'), may hold values from -0.125 to 0.125
- query_projection_matrix: bfloat16 [2048, 1024], P(None, 'tp'), may hold values from -0.125 to 0.125
- key_projection_matrix: bfloat16 [2048, 1024], P(None, 'tp'), may hold values from -0.125 to 0.125
- value_projection_matrix: bfloat16 [2048, 1024], P(None, 'tp'), may hold values from -0.125 to 0.125
- output_gate_matrix: bfloat16 [2048, 1024], P(None, 'tp'), may hold values from -0.125 to 0.125
- input_gate_matrix: bfloat16 [2048, 2, 8], replicated
- forget_gate_matrix: bfloat16 [2048, 2, 8], replicated, may hold values from -0.125 to 0.125
- forget_gate_bias: float32 [2, 8], replicated
- log_forget_scale: float32 [2, 8192], P(None, 'sp'), may hold values from 0.35 to 2.8
- extra_log_forget: float32 [2, 8192], P(None, 'sp'), may hold values from -0.7 to 0, as said below
- starting_memory: float32 [2, 8, 128, 128], P(None, 'tp'), may hold values from -3 to 3
- starting_normalizer: float32 [2, 8, 128], P(None, 'tp'), may hold values from -3 to 3
- starting_log_scale: float32 [2, 8], P(None, 'tp'), may hold values from 2 to 5
- pooling_group_map: bfloat16 [4, 128, 128], replicated, may hold values from -0.5 to 0.5
- pooling_channel_scale: float32 [512], replicated, may hold values from 0.1 to 1.9
- memory_head_gain: float32 [1024], replicated, may hold values from 0.1 to 1.9
- pooling_output_matrix: bfloat16 [512, 2048], replicated, may hold values from -0.25 to 0.25
- memory_output_matrix: bfloat16 [1024, 2048], replicated, may hold values from -0.1875 to 0.1875
Outputs:
- mixed_out: bfloat16 [8192, 2048], P(('sp', 'tp'))
The draws below stay inside these ranges and needn't reach their ends.
Inputs may be any that keep to these rules, and one draw needn't show every extreme that they name: `extra_log_forget`: at most three nonzero entries in each direction.
All inputs are finite; a program needn't handle non-finite values.
Results may differ from the reference program's by a relative error of at most 0.0091.
Values may be sent and summed in bfloat16 or wider, within the bound.
A program may use at most 128 MiB of HBM per device.

```python
import jax
import jax.numpy as jnp
from jax import lax

D = 2048
POOL_GROUPS = 4
GROUP_DIM = 128
HEADS = 8
DH = 128
BLOCK = 128
TOK_DEV = 1024
POOL_W = 512
MEM_W = 1024
TOKENS = 8192


def draw_forget_gate_bias(key, part):
    pick_key, slow_key, fast_key = jax.random.split(key, 3)
    slow_share = 0.5
    slow_heads = jax.random.uniform(pick_key, (2, HEADS)) < slow_share
    slow_bias = jnp.log(jnp.float32(TOKENS)) + jax.random.uniform(slow_key, (2, HEADS), minval=1.5, maxval=2.5)
    fast_bias = jax.random.uniform(fast_key, (2, HEADS), minval=3.8, maxval=4.8)
    return jnp.where(slow_heads, slow_bias, fast_bias).astype(jnp.float32)


def draw_log_forget_scale(key, part):
    block_key, rough_key = jax.random.split(key)
    segments = TOKENS // TOK_DEV
    block_factor = jnp.exp(jax.random.uniform(block_key, (2, segments, 1), minval=-0.69, maxval=0.69))
    rough_factor = jax.random.uniform(rough_key, (2, segments, TOK_DEV), minval=0.7, maxval=1.4)
    return (block_factor * rough_factor).reshape(2, TOKENS).astype(jnp.float32)


def draw_extra_log_forget(key, part):
    first_key, second_key, depth_key = jax.random.split(key, 3)
    first_places = jax.random.permutation(first_key, TOKENS)[:3]
    second_places = jax.random.permutation(second_key, TOKENS)[:3]
    places = jnp.stack([first_places, second_places]).astype(jnp.int32)
    depths = jnp.log(jax.random.uniform(depth_key, (2, 3), minval=0.5, maxval=0.8))
    direction_rows = jnp.arange(2)[:, None]
    return jnp.zeros((2, TOKENS), jnp.float32).at[direction_rows, places].set(depths)


def draw_input_gate_matrix(key, part):
    base_key = jax.random.fold_in(key, 0)
    weights = jax.random.normal(base_key, (D, 2, HEADS), jnp.float32) * D ** (-0.5)
    return weights.astype(jnp.bfloat16)


def block_levels(own_key, extent, cuts, smallest, top_value):
    def one(dim, parts):
        steps = jax.random.uniform(jax.random.fold_in(jax.random.fold_in(own_key, 6), dim), (parts,), jnp.float32, smallest / len(cuts), top_value / len(cuts))
        return jnp.repeat(jnp.exp(steps), extent[dim] // parts).reshape((-1,) + (1,) * (len(extent) - dim - 1))

    factor_of = one(*cuts[0])
    for cut in cuts[1:]:
        factor_of = factor_of * one(*cut)
    return factor_of


def gaussian(own_key, dims, deviation, bound, cuts=(), kind=jnp.bfloat16):
    array = jax.random.normal(own_key, dims, jnp.float32) * deviation
    if len(cuts) > 0:
        array = block_levels(own_key, dims, cuts, -0.22, 0.18) * array
    return jnp.clip(array, min=-bound, max=bound).astype(kind)


def setup_inputs(seed: int = 0) -> dict:
    keys = jax.random.split(jax.random.key(seed), 21)
    return {
        "tokens": gaussian(keys[0], (TOKENS, D), 1.0, 6.0, ((0, 8), (1, 4))),
        "input_norm_gain": jnp.clip(1.0 + 0.18 * jax.random.normal(keys[1], (D,), jnp.float32), 0.1, 1.9),
        "pooling_input_matrix": gaussian(keys[2], (D, POOL_W), D ** -0.5, 0.125, ((1, 4),)),
        "query_projection_matrix": gaussian(keys[3], (D, MEM_W), D ** -0.5, 0.125, ((1, 4),)),
        "key_projection_matrix": gaussian(keys[4], (D, MEM_W), D ** -0.5, 0.125, ((1, 4),)),
        "value_projection_matrix": gaussian(keys[5], (D, MEM_W), D ** -0.5, 0.125, ((1, 4),)),
        "output_gate_matrix": gaussian(keys[6], (D, MEM_W), D ** -0.5, 0.125, ((1, 4),)),
        "input_gate_matrix": draw_input_gate_matrix(jax.random.fold_in(keys[20], 71), 0),
        "forget_gate_matrix": gaussian(keys[8], (D, 2, HEADS), D ** -0.5, 0.125),
        "forget_gate_bias": draw_forget_gate_bias(jax.random.fold_in(keys[20], 71), 0),
        "log_forget_scale": draw_log_forget_scale(jax.random.fold_in(keys[20], 71), 0),
        "extra_log_forget": draw_extra_log_forget(jax.random.fold_in(keys[20], 71), 0),
        "starting_memory": gaussian(keys[12], (2, HEADS, DH, DH), 0.5, 3.0, ((1, 4),), jnp.float32),
        "starting_normalizer": gaussian(keys[13], (2, HEADS, DH), 0.5, 3.0, ((1, 4),), jnp.float32),
        "starting_log_scale": jnp.clip(2.0 + 3.0 * jax.random.uniform(keys[14], (2, HEADS), jnp.float32) ** block_levels(keys[14], (2, HEADS), ((1, 4),), -0.2, 0.2), 2.0, 5.0),
        "pooling_group_map": gaussian(keys[15], (POOL_GROUPS, GROUP_DIM, GROUP_DIM), GROUP_DIM ** -0.5, 0.5),
        "pooling_channel_scale": jnp.clip(1.0 + 0.18 * jax.random.normal(keys[16], (POOL_W,), jnp.float32), 0.1, 1.9),
        "memory_head_gain": jnp.clip(1.0 + 0.18 * jax.random.normal(keys[17], (MEM_W,), jnp.float32), 0.1, 1.9),
        "pooling_output_matrix": gaussian(keys[18], (POOL_W, D), POOL_W ** -0.5, 0.25),
        "memory_output_matrix": gaussian(keys[19], (MEM_W, D), MEM_W ** -0.5, 0.1875),
    }


NEG_BIG = -1e+30
LN_EPS = 1e-05
HEAD_EPS = 1e-06
HIGHEST = lax.Precision.HIGHEST

def block_step(carried, pieces):
    memory, normer, maxlog = carried
    q_blk, k_blk, v_blk, i_blk, f_blk = pieces
    lower_mask = jnp.tril(jnp.ones((BLOCK, BLOCK), dtype=bool))
    cumulative = jnp.cumsum(f_blk, axis=-1)
    exponent = jnp.where(lower_mask, cumulative[:, :, None] - cumulative[:, None, :] + i_blk[:, None, :], NEG_BIG)
    carried_log = cumulative + maxlog[:, None]
    row_max = jnp.maximum(carried_log, exponent.max(-1))
    fading = jnp.exp(carried_log - row_max)
    scores = jnp.einsum('htd,hsd->hts', q_blk, k_blk, precision=HIGHEST) * jnp.exp(exponent - row_max[:, :, None])
    numerator = fading[:, :, None] * jnp.einsum('hvk,htk->htv', memory, q_blk, precision=HIGHEST) + jnp.einsum('hts,hsv->htv', scores, v_blk, precision=HIGHEST)
    denominator = fading * jnp.einsum('hk,htk->ht', normer, q_blk, precision=HIGHEST) + scores.sum(-1)
    summed = cumulative[:, -1]
    weight_log = summed[:, None] - cumulative + i_blk
    new_max = jnp.maximum(summed + maxlog, weight_log.max(-1))
    carry_scale = jnp.exp(summed + maxlog - new_max)
    weights = jnp.exp(weight_log - new_max[:, None])
    memory = carry_scale[:, None, None] * memory + jnp.einsum('hsv,hsk->hvk', v_blk * weights[:, :, None], k_blk, precision=HIGHEST)
    normer = carry_scale[:, None] * normer + jnp.einsum('hs,hsk->hk', weights, k_blk, precision=HIGHEST)
    return ((memory, normer, new_max), (numerator, denominator, row_max))

def to_blocks(source):
    return jnp.moveaxis(source.reshape((source.shape[0], source.shape[1] // BLOCK, BLOCK) + source.shape[2:]), 1, 0)

def from_blocks(source):
    return jnp.moveaxis(source, 0, 1).reshape((source.shape[1], source.shape[0] * source.shape[2]) + source.shape[3:])

def memory_direction(query_heads, key_heads, value_heads, log_in, log_forget_gate, initial):
    finals, outputs = lax.scan(block_step, initial, tuple((to_blocks(member) for member in (query_heads, key_heads, value_heads, log_in, log_forget_gate))))
    numerator, denominator, row_max = (from_blocks(member) for member in outputs)
    return numerator / jnp.maximum(jnp.abs(denominator), 1.0)[:, :, None]

def reference(tokens, input_norm_gain, pooling_input_matrix, query_projection_matrix, key_projection_matrix, value_projection_matrix, output_gate_matrix, input_gate_matrix, forget_gate_matrix, forget_gate_bias, log_forget_scale, extra_log_forget, starting_memory, starting_normalizer, starting_log_scale, pooling_group_map, pooling_channel_scale, memory_head_gain, pooling_output_matrix, memory_output_matrix):
    total_rows = tokens.shape[0]
    model_width = tokens.shape[1]
    floats = tokens.astype(jnp.float32)
    mean_row = lax.optimization_barrier(jnp.sum(floats, axis=1)) / model_width
    square_mean = lax.optimization_barrier(jnp.sum(floats * floats, axis=1)) / model_width
    variance = square_mean - mean_row * mean_row
    normed = ((floats - mean_row[:, None]) * lax.rsqrt(variance + LN_EPS)[:, None] * input_norm_gain).astype(jnp.bfloat16)

    def project(weight):
        return jnp.dot(normed, weight, preferred_element_type=jnp.float32)
    pool_in = project(pooling_input_matrix).astype(jnp.bfloat16)
    queries = project(query_projection_matrix).astype(jnp.bfloat16)
    key_rows = project(key_projection_matrix).astype(jnp.bfloat16)
    value_rows = project(value_projection_matrix).astype(jnp.bfloat16)
    out_gate = project(output_gate_matrix).astype(jnp.bfloat16)
    in_pre = project(input_gate_matrix.reshape(model_width, 2 * HEADS)).reshape(total_rows, 2, HEADS)
    forget_gate_preact = project(forget_gate_matrix.reshape(model_width, 2 * HEADS)).reshape(total_rows, 2, HEADS)
    log_forget_gate = jax.nn.log_sigmoid(forget_gate_preact + forget_gate_bias[None]) * log_forget_scale.T[:, :, None] + extra_log_forget.T[:, :, None]

    def heads_of(source, factor):
        return (source.astype(jnp.float32) * factor).reshape(total_rows, HEADS, DH).transpose(1, 0, 2)
    query_heads = heads_of(queries, 1.0)
    key_heads = heads_of(key_rows, DH ** (-0.5))
    value_heads = heads_of(value_rows, 1.0)
    forward = memory_direction(query_heads, key_heads, value_heads, in_pre[:, 0].T, log_forget_gate[:, 0].T, (starting_memory[0], starting_normalizer[0], starting_log_scale[0]))
    backward = memory_direction(query_heads[:, ::-1], key_heads[:, ::-1], value_heads[:, ::-1], in_pre[:, 1].T[:, ::-1], log_forget_gate[:, 1].T[:, ::-1], (starting_memory[1], starting_normalizer[1], starting_log_scale[1]))
    hidden = forward + backward[:, ::-1]
    head_mean = lax.optimization_barrier(jnp.mean(hidden, axis=-1, keepdims=True))
    head_var = lax.optimization_barrier(jnp.mean(jnp.square(hidden - head_mean), axis=-1, keepdims=True))
    scaled = (hidden - head_mean) * lax.rsqrt(head_var + HEAD_EPS) * memory_head_gain.reshape(HEADS, DH)[:, None, :]
    mem_out = (scaled.transpose(1, 0, 2).reshape(total_rows, HEADS * DH) * jax.nn.sigmoid(out_gate.astype(jnp.float32))).astype(jnp.bfloat16)
    positions = jnp.arange(total_rows, dtype=jnp.int32)
    group_outs = []
    for group_index in range(POOL_GROUPS):
        half_span = 2 ** group_index
        grouped = pool_in[:, group_index * GROUP_DIM:(group_index + 1) * GROUP_DIM].astype(jnp.float32)
        padded = jnp.pad(grouped, ((half_span, half_span), (0, 0)))
        pooled = jnp.zeros_like(grouped)
        for offset in range(-half_span, half_span):
            pooled = pooled + padded[half_span + offset:half_span + offset + total_rows]
        upper_edge = jnp.minimum(positions + half_span, total_rows)
        lower_edge = jnp.maximum(positions - half_span, 0)
        counts = (upper_edge - lower_edge).astype(jnp.float32)
        contrast = (pooled / counts[:, None] - grouped).astype(jnp.bfloat16)
        mapped = jnp.dot(contrast, pooling_group_map[group_index], preferred_element_type=jnp.float32)
        group_outs.append((mapped * pooling_channel_scale[group_index * GROUP_DIM:(group_index + 1) * GROUP_DIM]).astype(jnp.bfloat16))
    pool_out = jnp.concatenate(group_outs, axis=1)
    mixed = jnp.dot(pool_out, pooling_output_matrix, preferred_element_type=jnp.float32) + jnp.dot(mem_out, memory_output_matrix, preferred_element_type=jnp.float32)
    return mixed.astype(jnp.bfloat16)
```

```python
import functools

import jax
import jax.numpy as jnp
from jax import lax
from jax.experimental import pallas as pl
from jax.experimental.pallas import tpu as pltpu
from jax.sharding import PartitionSpec as P

DH = 128
NEG_BIG = -1e30
LN_EPS = 1e-05
HEAD_EPS = 1e-06
RIM = 16
AUG = 144
VMEM = pltpu.VMEM
MESH = pl.DeviceIdType.MESH
F32 = jnp.float32
BF16 = jnp.bfloat16


def whole_vmem(count):
    return [pl.BlockSpec(memory_space=pltpu.VMEM)] * count


def project_kernel(
    tp_size, chunks,
    tokens_ref, gain_ref, wpg_hbm, wq_hbm, wk_hbm, wv_hbm, wo_hbm,
    pool_ref, gates_ref, q_ref, k_ref, v_ref, o_ref,
    held, normed, wpg, wq, wk, wv, wo,
    load_sem, far_send, far_recv, near_send, near_recv, pass_send, pass_recv,
):
    me = lax.axis_index("tp")
    far = lax.rem(me + tp_size // 2, tp_size)
    near = me + 1 - 2 * lax.rem(me, 2)
    diagonal = lax.rem(near + tp_size // 2, tp_size)
    barrier = pltpu.get_barrier_semaphore()
    for other in (far, near):
        pl.semaphore_signal(barrier, inc=1, device_id={"tp": other}, device_id_type=MESH)
    pl.semaphore_wait(barrier, 2)
    step = tokens_ref.shape[0] // chunks
    width = tokens_ref.shape[1]

    def remote(source, slot, rows, send, recv, other):
        return pltpu.make_async_remote_copy(
            src_ref=source.at[rows], dst_ref=held.at[slot, rows], send_sem=send, recv_sem=recv,
            device_id={"tp": other}, device_id_type=MESH,
        )

    spans = [pl.ds(c * step, step) for c in range(chunks)]
    to_far = [remote(tokens_ref, 1, s, far_send.at[c], far_recv.at[c], far) for c, s in enumerate(spans)]
    to_near = [remote(tokens_ref, 0, s, near_send.at[c], near_recv.at[c], near) for c, s in enumerate(spans)]
    onward = [
        remote(held.at[1], 2, s, pass_send.at[c], pass_recv.at[c], near) for c, s in enumerate(spans)
    ]
    for c in range(chunks):
        to_far[c].start()
    loads = [
        pltpu.make_async_copy(source, target, load_sem.at[i])
        for i, (source, target) in enumerate(
            ((wpg_hbm, wpg), (wq_hbm, wq), (wk_hbm, wk), (wv_hbm, wv), (wo_hbm, wo))
        )
    ]
    for load in loads:
        load.start()
    for c in range(chunks):
        to_near[c].start()
    owners = (me, near, far, diagonal)
    model_width = width * tp_size
    for c, rows in enumerate(spans):
        to_far[c].wait_recv()
        onward[c].start()
        to_near[c].wait_recv()
        onward[c].wait_recv()
        views = [tokens_ref[rows, :]] + [held[slot, rows, :] for slot in range(3)]
        total = jnp.zeros((step, 1), F32)
        square = jnp.zeros((step, 1), F32)
        for view in views:
            part = view.astype(F32)
            total = total + jnp.sum(part, axis=1, keepdims=True)
            square = square + jnp.sum(part * part, axis=1, keepdims=True)
        mean = total / model_width
        inverse = lax.rsqrt(square / model_width - mean * mean + LN_EPS)
        for view, owner in zip(views, owners):
            columns = pl.ds(pl.multiple_of(owner * width, width), width)
            normed[:, columns] = (
                (view.astype(F32) - mean) * inverse * gain_ref[:, columns]
            ).astype(BF16)
        if c == 0:
            for load in loads:
                load.wait()
        x = normed[...]
        both = jnp.dot(x, wpg[...], preferred_element_type=F32)
        pool_ref[rows, :] = both[:, : pool_ref.shape[1]].astype(BF16)
        gates_ref[rows, :] = both[:, pool_ref.shape[1] :]
        for weight, target in ((wq, q_ref), (wk, k_ref), (wv, v_ref), (wo, o_ref)):
            target[rows, :] = jnp.dot(x, weight[...], preferred_element_type=F32).astype(BF16)
    for c in range(chunks):
        to_far[c].wait_send()
        to_near[c].wait_send()
        onward[c].wait_send()


def scan_lanes(values, combine, neutral, forward_rows):
    lanes = values.shape[1]
    lane = lax.broadcasted_iota(jnp.int32, values.shape, 1)
    forward = lax.broadcasted_iota(jnp.int32, values.shape, 0) < forward_rows
    shift = 1
    while shift < lanes:
        low = jnp.where(lane >= shift, pltpu.roll(values, shift, 1), neutral)
        high = jnp.where(lane < lanes - shift, pltpu.roll(values, lanes - shift, 1), neutral)
        values = combine(values, jnp.where(forward, low, high))
        shift *= 2
    return values


def memory_kernel(
    sp_size, heads, blocks,
    pool_ref, gates_ref, q_ref, k_ref, v_ref, o_ref, scale_ref, extra_ref, bias_ref,
    start_mem, start_norm, start_log, map_ref, pscale_ref, hgain_ref,
    out_ref,
    states, a_ref, acol_ref, locals_ref, inc_t, inc_s, exc_t, exc_s,
    send_t, send_s, recv_t, recv_s, rims, ext,
    ts, tr, ss, sr, rs, rr,
):
    me = lax.axis_index("sp")
    group = lax.axis_index("tp")
    rows_total = q_ref.shape[0]
    size = rows_total // blocks
    pairs = 2 * heads
    strides = []
    stride = 1
    while stride < sp_size:
        strides.append(stride)
        stride *= 2
    barrier = pltpu.get_barrier_semaphore()
    for stride in strides:
        for okay, other in ((me + stride < sp_size, me + stride), (me >= stride, me - stride)):
            @pl.when(okay)
            def _():
                pl.semaphore_signal(barrier, inc=1, device_id={"sp": other}, device_id_type=MESH)

    turned = jnp.transpose(gates_ref[...])
    log_in = turned[0:pairs]
    pre = turned[pairs : 2 * pairs] + bias_ref[...]
    log_sig = jnp.minimum(pre, 0.0) - jnp.log1p(jnp.exp(-jnp.abs(pre)))
    per_row = lambda ref: jnp.concatenate(
        [jnp.broadcast_to(ref[r : r + 1, :], (heads, rows_total)) for r in range(2)], axis=0
    )
    log_fg = log_sig * per_row(scale_ref) + per_row(extra_ref)
    falls = scan_lanes(log_fg, jnp.add, 0.0, heads)
    lifted = log_in - falls
    peaks = scan_lanes(lifted, jnp.maximum, NEG_BIG, heads)
    a_ref[...] = lifted + jnp.log(F32(DH ** -0.5))
    acol_ref[...] = jnp.transpose(
        jnp.concatenate([peaks, jnp.zeros((128 - pairs, rows_total), F32)], axis=0)
    )

    for h in range(heads):
        cols = slice(h * DH, (h + 1) * DH)
        vt = jnp.concatenate(
            [jnp.transpose(v_ref[:, cols].astype(F32)), jnp.ones((AUG - DH, rows_total), F32)], axis=0
        )
        for r in range(2):
            p = r * heads + h
            state = None
            before = None
            for n in range(blocks):
                b = n if r == 0 else blocks - 1 - n
                span = slice(b * size, (b + 1) * size)
                last = (b + 1) * size - 1 if r == 0 else b * size
                after = peaks[p : p + 1, last : last + 1]
                weight = jnp.exp(a_ref[p : p + 1, span] - after)
                add = jnp.dot(
                    (vt[:, span] * weight).astype(BF16), k_ref[span, cols], preferred_element_type=F32
                )
                if n > 0:
                    states[p, b] = state
                    state = jnp.exp(before - after) * state + add
                else:
                    state = add
                before = after
            end = rows_total - 1 if r == 0 else 0
            fall = falls[p : p + 1, end : end + 1]
            inc_t[p] = state
            inc_s[r, h : h + 1, :] = jnp.broadcast_to(before + fall, (1, 128))
            inc_s[r, heads + h : heads + h + 1, :] = jnp.broadcast_to(fall, (1, 128))
            exc_t[p] = jnp.zeros((AUG, DH), F32)
            exc_s[r, h : h + 1, :] = jnp.full((1, 128), NEG_BIG, F32)
            exc_s[r, heads + h : heads + h + 1, :] = jnp.zeros((1, 128), F32)

    peers = jnp.int32(0)
    for stride in strides:
        peers = peers + (me + stride < sp_size).astype(jnp.int32) + (me >= stride).astype(jnp.int32)
    pl.semaphore_wait(barrier, peers)

    def copies(level, r, other):
        t = pltpu.make_async_remote_copy(
            src_ref=send_t.at[level, r], dst_ref=recv_t.at[level, r], send_sem=ts.at[level, r],
            recv_sem=tr.at[level, r], device_id={"sp": other}, device_id_type=MESH,
        )
        s = pltpu.make_async_remote_copy(
            src_ref=send_s.at[level, r], dst_ref=recv_s.at[level, r], send_sem=ss.at[level, r],
            recv_sem=sr.at[level, r], device_id={"sp": other}, device_id_type=MESH,
        )
        return (t, s)

    def ends(level, r):
        stride = strides[level]
        if r == 0:
            return (me + stride < sp_size, me + stride, me >= stride)
        return (me >= stride, me - stride, me + stride < sp_size)

    def send(level):
        for r in range(2):
            okay, other, _unused = ends(level, r)
            send_s[level, r] = inc_s[r]
            for h in range(heads):
                send_t[level, r, h] = inc_t[r * heads + h].astype(BF16)

            @pl.when(okay)
            def _():
                for copy in copies(level, r, other):
                    copy.start()

    def fold(level, r, t_ref, s_ref):
        for h in range(heads):
            p = r * heads + h
            early_max = recv_s[level, r, h : h + 1, :]
            early_fall = recv_s[level, r, heads + h : heads + h + 1, :]
            late_max = s_ref[r, h : h + 1, :]
            late_fall = s_ref[r, heads + h : heads + h + 1, :]
            top = jnp.maximum(early_max + late_fall, late_max)
            t_ref[p] = (
                jnp.exp(early_max + late_fall - top) * recv_t[level, r, h].astype(F32)
                + jnp.exp(late_max - top) * t_ref[p]
            )
            s_ref[r, h : h + 1, :] = top
            s_ref[r, heads + h : heads + h + 1, :] = early_fall + late_fall

    def receive(level):
        for r in range(2):
            okay, other, has = ends(level, r)

            @pl.when(has)
            def _():
                for copy in copies(level, r, other):
                    copy.wait_recv()
                fold(level, r, exc_t, exc_s)
                if level + 1 < len(strides):
                    fold(level, r, inc_t, inc_s)

    def rim(side):
        rows = pl.ds(rows_total - RIM, RIM) if side == 0 else pl.ds(0, RIM)
        other = me + 1 if side == 0 else me - 1
        return pltpu.make_async_remote_copy(
            src_ref=pool_ref.at[rows], dst_ref=rims.at[side], send_sem=rs.at[side],
            recv_sem=rr.at[side], device_id={"sp": other}, device_id_type=MESH,
        )

    rim_sends = (me + 1 < sp_size, me >= 1)
    rim_recvs = (me >= 1, me + 1 < sp_size)

    def local_head(h):
        cols = slice(h * DH, (h + 1) * DH)
        t_at = lax.broadcasted_iota(jnp.int32, (size, size), 0)
        s_at = lax.broadcasted_iota(jnp.int32, (size, size), 1)
        for b in range(blocks):
            span = slice(b * size, (b + 1) * size)
            queries = q_ref[span, cols]
            scores = lax.dot_general(
                queries, k_ref[span, cols], (((1,), (1,)), ((), ())), preferred_element_type=F32
            )
            values = jnp.concatenate([v_ref[span, cols], jnp.ones((size, DH), BF16)], axis=1)
            for r in range(2):
                p = r * heads + h
                peak = acol_ref[span, p : p + 1]
                inside = (s_at <= t_at) if r == 0 else (s_at >= t_at)
                weight = jnp.exp(jnp.where(inside, a_ref[p : p + 1, span] - peak, NEG_BIG))
                part = jnp.dot((scores * weight).astype(BF16), values, preferred_element_type=F32)
                inner = b > 0 if r == 0 else b < blocks - 1
                if inner:
                    edge = b * size - 1 if r == 0 else (b + 1) * size
                    base = acol_ref[edge : edge + 1, p : p + 1]
                    part = part + jnp.exp(base - peak) * against(queries, states[p, b])
                locals_ref[p, span, :] = part

    def against(queries, state):
        spread = jnp.concatenate(
            [state[:DH], jnp.broadcast_to(state[DH : DH + 1], (DH, DH))], axis=0
        ).astype(BF16)
        return lax.dot_general(
            queries, spread, (((1,), (1,)), ((), ())), preferred_element_type=F32
        )

    def pooling():
        for side in range(2):
            @pl.when(rim_recvs[side])
            def _():
                rim(side).wait_recv()
                at = 0 if side == 0 else RIM + rows_total
                ext[at : at + RIM, :] = rims[side].astype(F32)

            @pl.when(jnp.logical_not(rim_recvs[side]))
            def _():
                at = 0 if side == 0 else RIM + rows_total
                ext[at : at + RIM, :] = jnp.zeros((RIM, ext.shape[1]), F32)
        own = pool_ref[...].astype(F32)
        ext[RIM : RIM + rows_total, :] = own
        half = jnp.left_shift(jnp.int32(1), group)
        pooled = jnp.zeros_like(own)
        reach = RIM // 2
        for offset in range(-reach, reach):
            use = jnp.logical_and(offset >= -half, offset < half).astype(F32)
            pooled = pooled + use * ext[RIM + offset : RIM + offset + rows_total, :]
        position = me * rows_total + lax.broadcasted_iota(jnp.int32, own.shape, 0)
        count = jnp.minimum(position + half, rows_total * sp_size) - jnp.maximum(position - half, 0)
        contrast = (pooled / count.astype(F32) - own).astype(BF16)
        mapped = jnp.dot(contrast, map_ref[...], preferred_element_type=F32)
        width = map_ref.shape[1]
        out_ref[:, :width] = (mapped * pscale_ref[...]).astype(BF16)

    for side in range(2):
        @pl.when(rim_sends[side])
        def _():
            rim(side).start()

    work = [functools.partial(local_head, h) for h in range(heads)] + [pooling]
    for level in range(len(strides)):
        send(level)
        if work:
            work.pop(0)()
        receive(level)
    for item in work:
        item()

    width = map_ref.shape[1]
    for h in range(heads):
        cols = slice(h * DH, (h + 1) * DH)
        enter = []
        for r in range(2):
            p = r * heads + h
            begin = start_log[p : p + 1, :]
            late_max = exc_s[r, h : h + 1, :]
            late_fall = exc_s[r, heads + h : heads + h + 1, :]
            top = jnp.maximum(begin + late_fall, late_max)
            early = jnp.exp(begin + late_fall - top)
            late = jnp.exp(late_max - top)
            mem = early * start_mem[p] + late * exc_t[p, :DH, :]
            norm = early * start_norm[p : p + 1, :] + late * exc_t[p, DH : DH + 1, :]
            enter.append(
                (jnp.concatenate([mem, jnp.broadcast_to(norm, (DH, DH))], axis=0).astype(BF16), top[:, 0:1])
            )
        for b in range(blocks):
            span = slice(b * size, (b + 1) * size)
            queries = q_ref[span, cols]
            hidden = jnp.zeros((size, DH), F32)
            for r in range(2):
                p = r * heads + h
                spread, top = enter[r]
                peak = acol_ref[span, p : p + 1]
                joint = jnp.maximum(peak, top)
                full = jnp.exp(peak - joint) * locals_ref[p, span, :] + jnp.exp(
                    top - joint
                ) * lax.dot_general(
                    queries, spread, (((1,), (1,)), ((), ())), preferred_element_type=F32
                )
                hidden = hidden + full[:, :DH] / jnp.maximum(jnp.abs(full[:, DH:]), 1.0)
            centered = hidden - jnp.mean(hidden, axis=1, keepdims=True)
            spread_sq = jnp.mean(centered * centered, axis=1, keepdims=True)
            gate = 1.0 / (1.0 + jnp.exp(-o_ref[span, cols].astype(F32)))
            out_ref[span, width + h * DH : width + (h + 1) * DH] = (
                centered * lax.rsqrt(spread_sq + HEAD_EPS) * hgain_ref[:, cols] * gate
            ).astype(BF16)

    for level in range(len(strides)):
        for r in range(2):
            okay, other, _unused = ends(level, r)

            @pl.when(okay)
            def _():
                for copy in copies(level, r, other):
                    copy.wait_send()
    for side in range(2):
        @pl.when(rim_sends[side])
        def _():
            rim(side).wait_send()


def per_device(
    tokens,
    input_norm_gain,
    pooling_input_matrix,
    query_projection_matrix,
    key_projection_matrix,
    value_projection_matrix,
    output_gate_matrix,
    input_gate_matrix,
    forget_gate_matrix,
    forget_gate_bias,
    log_forget_scale,
    extra_log_forget,
    starting_memory,
    starting_normalizer,
    starting_log_scale,
    pooling_group_map,
    pooling_channel_scale,
    memory_head_gain,
    pooling_output_matrix,
    memory_output_matrix,
):
    rows, own_width = tokens.shape
    tp_size = lax.axis_size("tp")
    sp_size = lax.axis_size("sp")
    model_width = own_width * tp_size
    group = lax.axis_index("tp")
    group_dim = pooling_input_matrix.shape[1]
    heads = query_projection_matrix.shape[1] // DH
    mem_width = heads * DH
    pairs = 2 * heads
    gate_in = lax.dynamic_slice_in_dim(input_gate_matrix, group * heads, heads, 2)
    gate_fg = lax.dynamic_slice_in_dim(forget_gate_matrix, group * heads, heads, 2)
    gate_weight = jnp.concatenate([gate_in, gate_fg], axis=1).reshape(model_width, 2 * pairs)
    wpg = jnp.concatenate(
        [pooling_input_matrix, gate_weight, jnp.zeros((model_width, 128 - 2 * pairs), BF16)], axis=1
    )
    chunks = 4
    anywhere = pl.BlockSpec(memory_space=pl.ANY)
    pool_in, gates, queries, keys, values, out_gate = pl.pallas_call(
        functools.partial(project_kernel, tp_size, chunks),
        out_shape=[
            jax.ShapeDtypeStruct((rows, group_dim), BF16),
            jax.ShapeDtypeStruct((rows, 128), F32),
        ]
        + [jax.ShapeDtypeStruct((rows, mem_width), BF16)] * 4,
        in_specs=whole_vmem(2) + [anywhere] * 5,
        out_specs=whole_vmem(6),
        scratch_shapes=[
            VMEM((3, rows, own_width), BF16),
            VMEM((rows // chunks, model_width), BF16),
            VMEM((model_width, group_dim + 128), BF16),
        ]
        + [VMEM((model_width, mem_width), BF16)] * 4
        + [pltpu.SemaphoreType.DMA((5,))]
        + [pltpu.SemaphoreType.DMA((chunks,))] * 6,
        compiler_params=pltpu.CompilerParams(
            collective_id=0, has_side_effects=True, vmem_limit_bytes=48 * 1024 * 1024
        ),
    )(
        tokens,
        input_norm_gain.reshape(1, model_width),
        wpg,
        query_projection_matrix,
        key_projection_matrix,
        value_projection_matrix,
        output_gate_matrix,
    )
    bias = lax.dynamic_slice_in_dim(forget_gate_bias, group * heads, heads, 1).reshape(pairs, 1)
    start_log = jnp.broadcast_to(starting_log_scale.reshape(pairs, 1), (pairs, 128))
    map_own = lax.dynamic_index_in_dim(pooling_group_map, group, 0, keepdims=False)
    pscale = lax.dynamic_slice_in_dim(pooling_channel_scale, group * group_dim, group_dim, 0)
    hgain = lax.dynamic_slice_in_dim(memory_head_gain, group * mem_width, mem_width, 0)
    levels = max(1, (sp_size - 1).bit_length())
    blocks = rows // 256
    mixed = pl.pallas_call(
        functools.partial(memory_kernel, sp_size, heads, blocks),
        out_shape=jax.ShapeDtypeStruct((rows, group_dim + mem_width), BF16),
        in_specs=whole_vmem(15),
        out_specs=pl.BlockSpec(memory_space=pltpu.VMEM),
        scratch_shapes=[
            VMEM((pairs, blocks, AUG, DH), F32),
            VMEM((pairs, rows), F32),
            VMEM((rows, 128), F32),
            VMEM((pairs, rows, 2 * DH), F32),
            VMEM((pairs, AUG, DH), F32),
            VMEM((2, 2 * heads, 128), F32),
            VMEM((pairs, AUG, DH), F32),
            VMEM((2, 2 * heads, 128), F32),
            VMEM((levels, 2, heads, AUG, DH), BF16),
            VMEM((levels, 2, 2 * heads, 128), F32),
            VMEM((levels, 2, heads, AUG, DH), BF16),
            VMEM((levels, 2, 2 * heads, 128), F32),
            VMEM((2, RIM, group_dim), BF16),
            VMEM((rows + 2 * RIM, group_dim), F32),
        ]
        + [pltpu.SemaphoreType.DMA((levels, 2))] * 4
        + [pltpu.SemaphoreType.DMA((2,))] * 2,
        compiler_params=pltpu.CompilerParams(
            collective_id=1, has_side_effects=True, vmem_limit_bytes=48 * 1024 * 1024
        ),
    )(
        pool_in,
        gates,
        queries,
        keys,
        values,
        out_gate,
        log_forget_scale,
        extra_log_forget,
        bias,
        starting_memory.reshape(pairs, DH, DH),
        starting_normalizer.reshape(pairs, DH),
        start_log,
        map_own,
        pscale.reshape(1, group_dim),
        hgain.reshape(1, mem_width),
    )
    owned = lax.all_to_all(mixed, "tp", split_axis=0, concat_axis=1, tiled=True)
    owner_rows = owned.shape[0]
    owned = owned.reshape(owner_rows, tp_size, group_dim + mem_width)
    pool_part = owned[:, :, :group_dim].reshape(owner_rows, tp_size * group_dim)
    mem_part = owned[:, :, group_dim:].reshape(owner_rows, tp_size * mem_width)
    result = jnp.dot(
        pool_part, pooling_output_matrix, preferred_element_type=F32
    ) + jnp.dot(mem_part, memory_output_matrix, preferred_element_type=F32)
    return result.astype(BF16)


def solution(mesh):
    placed = (
        P("sp", "tp"),
        P(),
        P(None, "tp"),
        P(None, "tp"),
        P(None, "tp"),
        P(None, "tp"),
        P(None, "tp"),
        P(),
        P(),
        P(),
        P(None, "sp"),
        P(None, "sp"),
        P(None, "tp", None, None),
        P(None, "tp", None),
        P(None, "tp"),
        P(),
        P(),
        P(),
        P(),
        P(),
    )
    return jax.shard_map(
        per_device, mesh=mesh, in_specs=placed, out_specs=P(("sp", "tp"), None), check_vma=False
    )
```

```python
import functools

import jax
import jax.numpy as jnp
from jax import lax
from jax.experimental import pallas as pl
from jax.experimental.pallas import tpu as pltpu
from jax.sharding import PartitionSpec as P

DH = 128
NEG_BIG = -1e30
LN_EPS = 1e-05
HEAD_EPS = 1e-06
RIM = 16
AUG = 144
VMEM = pltpu.VMEM
MESH = pl.DeviceIdType.MESH
F32 = jnp.float32
BF16 = jnp.bfloat16


def whole_vmem(count):
    return [pl.BlockSpec(memory_space=pltpu.VMEM)] * count


def scan_lanes(values, combine, neutral, forward_rows):
    lanes = values.shape[1]
    lane = lax.broadcasted_iota(jnp.int32, values.shape, 1)
    forward = lax.broadcasted_iota(jnp.int32, values.shape, 0) < forward_rows
    shift = 1
    while shift < lanes:
        low = jnp.where(lane >= shift, pltpu.roll(values, shift, 1), neutral)
        high = jnp.where(lane < lanes - shift, pltpu.roll(values, lanes - shift, 1), neutral)
        values = combine(values, jnp.where(forward, low, high))
        shift *= 2
    return values


def layer_kernel(
    tp_size, sp_size, heads,
    tokens_ref, gain_ref, gin_ref, gfg_ref, scale_ref, extra_ref, bias_ref,
    start_mem, start_norm, start_log, map_ref, pscale_ref, hgain_ref,
    wp_hbm, wq_hbm, wk_hbm, wv_hbm, wo_hbm, wpo_hbm, wmo_hbm,
    out_ref,
    held, normed, gate_w, wp, wq, wk, wv, wo, wpo, wmo,
    ext, q_ref, k_ref, v_ref, o_ref, gates_ref,
    adds, a_ref, acol_ref, ends_ref, locals_ref, inc_t, inc_s, exc_t, exc_s,
    send_t, send_s, recv_t, recv_s, rim_out, rims, enter_t, enter_s,
    pool_out, mem_out, lhs_pool, lhs_mem, acc,
    load_sem, far_send, far_recv, near_send, near_recv, pass_send, pass_recv,
    ts, tr, ss, sr, rs, rr, ps, pr, ms, mr,
):
    me = lax.axis_index("sp")
    group = lax.axis_index("tp")
    far = lax.rem(group + tp_size // 2, tp_size)
    near = group + 1 - 2 * lax.rem(group, 2)
    diagonal = lax.rem(near + tp_size // 2, tp_size)
    others = (far, diagonal, near)
    rows_total, width = tokens_ref.shape
    model_width = width * tp_size
    blocks = tp_size
    size = rows_total // blocks
    pairs = 2 * heads
    all_heads = gin_ref.shape[1]
    group_dim = map_ref.shape[1]
    mem_width = heads * DH
    strides = []
    stride = 1
    while stride < sp_size:
        strides.append(stride)
        stride *= 2

    barrier = pltpu.get_barrier_semaphore()
    peers = jnp.int32(len(others))
    for other in others:
        pl.semaphore_signal(barrier, inc=1, device_id={"tp": other}, device_id_type=MESH)
    for stride in strides:
        for okay, other in ((me + stride < sp_size, me + stride), (me >= stride, me - stride)):
            peers = peers + okay.astype(jnp.int32)

            @pl.when(okay)
            def _():
                pl.semaphore_signal(barrier, inc=1, device_id={"sp": other}, device_id_type=MESH)

    def load_group(pairs_of, first):
        copies = [
            pltpu.make_async_copy(source, target, load_sem.at[first + i])
            for i, (source, target) in enumerate(pairs_of)
        ]
        for copy in copies:
            copy.start()
        return copies

    loads = load_group(((wp_hbm, wp), (wq_hbm, wq), (wk_hbm, wk), (wv_hbm, wv), (wo_hbm, wo)), 0)
    gate_w[...] = jnp.concatenate(
        [ref[r].astype(F32) for ref in (gin_ref, gfg_ref) for r in range(2)], axis=0
    ).astype(BF16)
    pl.semaphore_wait(barrier, peers)

    def to_tp(source, target, send, recv, other):
        return pltpu.make_async_remote_copy(
            src_ref=source, dst_ref=target, send_sem=send, recv_sem=recv,
            device_id={"tp": other}, device_id_type=MESH,
        )

    def to_sp(source, target, send, recv, other):
        return pltpu.make_async_remote_copy(
            src_ref=source, dst_ref=target, send_sem=send, recv_sem=recv,
            device_id={"sp": other}, device_id_type=MESH,
        )

    spans = [pl.ds(c * size, size) for c in range(blocks)]
    to_far = [
        to_tp(tokens_ref.at[s], held.at[1, s], far_send.at[c], far_recv.at[c], far)
        for c, s in enumerate(spans)
    ]
    to_near = [
        to_tp(tokens_ref.at[s], held.at[0, s], near_send.at[c], near_recv.at[c], near)
        for c, s in enumerate(spans)
    ]
    onward = [
        to_tp(held.at[1, s], held.at[2, s], pass_send.at[c], pass_recv.at[c], near)
        for c, s in enumerate(spans)
    ]
    for c in range(blocks):
        to_far[c].start()
    for c in range(blocks):
        to_near[c].start()
    late_loads = load_group(((wpo_hbm, wpo), (wmo_hbm, wmo)), 5)

    bias_lane = lax.broadcasted_iota(jnp.int32, bias_ref.shape, 1)
    picked = [
        jnp.sum(jnp.where(bias_lane == group * heads + h, bias_ref[...], 0.0), axis=1, keepdims=True)
        for h in range(heads)
    ]
    bias = jnp.concatenate([picked[h][r : r + 1] for r in range(2) for h in range(heads)], axis=0)

    def own_gates(kind):
        parts = []
        for r in range(2):
            base = (2 * kind + r) * all_heads
            mine = gates_ref[base : base + heads, :]
            for other in range(1, tp_size):
                at = base + other * heads
                mine = jnp.where(group == other, gates_ref[at : at + heads, :], mine)
            parts.append(mine)
        return jnp.concatenate(parts, axis=0)

    def both_rows(ref, span):
        return jnp.concatenate(
            [jnp.broadcast_to(ref[r : r + 1, span], (heads, size)) for r in range(2)], axis=0
        )

    def project(c):
        rows = spans[c]
        views = [tokens_ref[rows, :]] + [held[slot, rows, :] for slot in range(3)]
        total = jnp.zeros((size, 1), F32)
        square = jnp.zeros((size, 1), F32)
        for view in views:
            part = view.astype(F32)
            total = total + jnp.sum(part, axis=1, keepdims=True)
            square = square + jnp.sum(part * part, axis=1, keepdims=True)
        mean = total / model_width
        inverse = lax.rsqrt(square / model_width - mean * mean + LN_EPS)
        for view, owner in zip(views, (group, near, far, diagonal)):
            columns = pl.ds(pl.multiple_of(owner * width, width), width)
            normed[:, columns] = (
                (view.astype(F32) - mean) * inverse * gain_ref[:, columns]
            ).astype(BF16)
        if c == 0:
            for load in loads:
                load.wait()
        x = normed[...]
        for weight, target in ((wk, k_ref), (wv, v_ref), (wq, q_ref), (wo, o_ref)):
            target[rows, :] = jnp.dot(x, weight[...], preferred_element_type=F32).astype(BF16)
        gates_ref[...] = lax.dot_general(
            gate_w[...], x, (((1,), (1,)), ((), ())), preferred_element_type=F32
        )
        pool = jnp.dot(x, wp[...], preferred_element_type=F32).astype(BF16)
        ext[pl.ds(RIM + c * size, size), :] = pool.astype(F32)
        if c == 0:
            rim_out[1] = pool[:RIM]
        if c == blocks - 1:
            rim_out[0] = pool[size - RIM :]

    def local_block(b):
        span = slice(b * size, (b + 1) * size)
        pre = own_gates(1) + bias
        log_sig = jnp.minimum(pre, 0.0) - jnp.log1p(jnp.exp(-jnp.abs(pre)))
        log_fg = log_sig * both_rows(scale_ref, span) + both_rows(extra_ref, span)
        falls = scan_lanes(log_fg, jnp.add, 0.0, heads)
        lifted = own_gates(0) - falls
        peaks = scan_lanes(lifted, jnp.maximum, NEG_BIG, heads)
        sources = lifted + jnp.log(F32(DH ** -0.5))
        columns = jnp.transpose(
            jnp.concatenate([peaks, jnp.zeros((128 - pairs, size), F32)], axis=0)
        )
        acol_ref[span, :] = columns
        t_at = lax.broadcasted_iota(jnp.int32, (size, size), 0)
        s_at = lax.broadcasted_iota(jnp.int32, (size, size), 1)
        for h in range(heads):
            cols = slice(h * DH, (h + 1) * DH)
            keys = k_ref[span, cols]
            vt = jnp.concatenate(
                [jnp.transpose(v_ref[span, cols].astype(F32)), jnp.ones((AUG - DH, size), F32)], axis=0
            )
            scores = lax.dot_general(
                q_ref[span, cols], keys, (((1,), (1,)), ((), ())), preferred_element_type=F32
            )
            values = jnp.concatenate([v_ref[span, cols], jnp.ones((size, DH), BF16)], axis=1)
            for r in range(2):
                p = r * heads + h
                end = size - 1 if r == 0 else 0
                top = peaks[p : p + 1, end : end + 1]
                ends_ref[b, p : p + 1, :] = jnp.broadcast_to(top, (1, 128))
                ends_ref[b, pairs + p : pairs + p + 1, :] = jnp.broadcast_to(
                    falls[p : p + 1, end : end + 1], (1, 128)
                )
                adds[p, b] = jnp.dot(
                    (vt * jnp.exp(sources[p : p + 1] - top)).astype(BF16), keys,
                    preferred_element_type=F32,
                )
                inside = (s_at <= t_at) if r == 0 else (s_at >= t_at)
                weight = jnp.exp(
                    jnp.where(inside, sources[p : p + 1] - columns[:, p : p + 1], NEG_BIG)
                )
                locals_ref[p, span, :] = jnp.dot(
                    (scores * weight).astype(BF16), values, preferred_element_type=F32
                )

    for c in range(blocks):
        to_far[c].wait_recv()
        onward[c].start()
        to_near[c].wait_recv()
        onward[c].wait_recv()
        project(c)
        local_block(c)

    def advance(p, b, state, level):
        peak = ends_ref[b, p : p + 1, :]
        fall = ends_ref[b, pairs + p : pairs + p + 1, :]
        top = jnp.maximum(level, peak)
        state = jnp.exp(level - top) * state + jnp.exp(peak - top) * adds[p, b]
        return (state, top + fall, fall)

    order = (tuple(range(blocks)), tuple(reversed(range(blocks))))
    for r in range(2):
        for h in range(heads):
            p = r * heads + h
            state = jnp.zeros((AUG, DH), F32)
            level = jnp.full((1, 128), NEG_BIG, F32)
            total_fall = jnp.zeros((1, 128), F32)
            for b in order[r]:
                state, level, fall = advance(p, b, state, level)
                total_fall = total_fall + fall
            inc_t[p] = state
            inc_s[r, h : h + 1, :] = level
            inc_s[r, heads + h : heads + h + 1, :] = total_fall
            exc_t[p] = jnp.zeros((AUG, DH), F32)
            exc_s[r, h : h + 1, :] = jnp.full((1, 128), NEG_BIG, F32)
            exc_s[r, heads + h : heads + h + 1, :] = jnp.zeros((1, 128), F32)

    def copies(level, r, other):
        return (
            to_sp(send_t.at[level, r], recv_t.at[level, r], ts.at[level, r], tr.at[level, r], other),
            to_sp(send_s.at[level, r], recv_s.at[level, r], ss.at[level, r], sr.at[level, r], other),
        )

    def route(level, r):
        stride = strides[level]
        if r == 0:
            return (me + stride < sp_size, me + stride, me >= stride)
        return (me >= stride, me - stride, me + stride < sp_size)

    def send(level):
        for r in range(2):
            okay, other, _unused = route(level, r)
            send_s[level, r] = inc_s[r]
            for h in range(heads):
                send_t[level, r, h] = inc_t[r * heads + h].astype(BF16)

            @pl.when(okay)
            def _():
                for copy in copies(level, r, other):
                    copy.start()

    def fold(level, r, t_ref, s_ref):
        for h in range(heads):
            p = r * heads + h
            early_max = recv_s[level, r, h : h + 1, :]
            early_fall = recv_s[level, r, heads + h : heads + h + 1, :]
            late_max = s_ref[r, h : h + 1, :]
            late_fall = s_ref[r, heads + h : heads + h + 1, :]
            top = jnp.maximum(early_max + late_fall, late_max)
            t_ref[p] = (
                jnp.exp(early_max + late_fall - top) * recv_t[level, r, h].astype(F32)
                + jnp.exp(late_max - top) * t_ref[p]
            )
            s_ref[r, h : h + 1, :] = top
            s_ref[r, heads + h : heads + h + 1, :] = early_fall + late_fall

    def receive(level, t_ref, s_ref, first):
        for r in range(2):
            okay, other, has = route(level, r)

            @pl.when(has)
            def _():
                if first:
                    for copy in copies(level, r, other):
                        copy.wait_recv()
                fold(level, r, t_ref, s_ref)

    def rim(side):
        other = me + 1 if side == 0 else me - 1
        return to_sp(rim_out.at[side], rims.at[side], rs.at[side], rr.at[side], other)

    rim_sends = (me + 1 < sp_size, me >= 1)
    rim_recvs = (me >= 1, me + 1 < sp_size)

    def pooling():
        for side in range(2):
            at = 0 if side == 0 else RIM + rows_total

            @pl.when(rim_recvs[side])
            def _():
                rim(side).wait_recv()
                ext[at : at + RIM, :] = rims[side].astype(F32)

            @pl.when(jnp.logical_not(rim_recvs[side]))
            def _():
                ext[at : at + RIM, :] = jnp.zeros((RIM, group_dim), F32)
        own = ext[RIM : RIM + rows_total, :]
        half = jnp.left_shift(jnp.int32(1), group)
        pooled = jnp.zeros_like(own)
        reach = RIM // 2
        for offset in range(-reach, reach):
            use = jnp.logical_and(offset >= -half, offset < half).astype(F32)
            pooled = pooled + use * ext[RIM + offset : RIM + offset + rows_total, :]
        position = me * rows_total + lax.broadcasted_iota(jnp.int32, own.shape, 0)
        count = jnp.minimum(position + half, rows_total * sp_size) - jnp.maximum(position - half, 0)
        contrast = (pooled / count.astype(F32) - own).astype(BF16)
        mapped = jnp.dot(contrast, map_ref[group], preferred_element_type=F32)
        scale = pscale_ref[:, pl.ds(pl.multiple_of(group * group_dim, group_dim), group_dim)]
        pool_out[...] = (mapped * scale).astype(BF16)

    pool_cols = pl.ds(pl.multiple_of(group * group_dim, group_dim), group_dim)
    mem_cols = pl.ds(pl.multiple_of(group * mem_width, mem_width), mem_width)

    def rows_of(owner):
        return pl.ds(pl.multiple_of(owner * size, size), size)

    pool_copies = [
        to_tp(pool_out.at[rows_of(other)], lhs_pool.at[:, pool_cols], ps.at[j], pr.at[j], other)
        for j, other in enumerate(others)
    ]
    mem_copies = [
        to_tp(mem_out.at[rows_of(other)], lhs_mem.at[:, mem_cols], ms.at[j], mr.at[j], other)
        for j, other in enumerate(others)
    ]

    def pool_product():
        lhs_pool[:, pool_cols] = pool_out[rows_of(group), :]
        for copy in pool_copies:
            copy.wait_recv()
        for load in late_loads:
            load.wait()
        acc[...] = jnp.dot(lhs_pool[...], wpo[...], preferred_element_type=F32)

    def start_pool():
        pooling()
        for copy in pool_copies:
            copy.start()

    send(0)
    for side in range(2):
        @pl.when(rim_sends[side])
        def _():
            rim(side).start()
    between = [start_pool] + [lambda: None] * len(strides)
    if len(strides) > 1:
        between[len(strides) - 1] = pool_product
    for level in range(len(strides)):
        if level > 0:
            send(level)
            receive(level - 1, exc_t, exc_s, False)
        between[level]()
        if level + 1 < len(strides):
            receive(level, inc_t, inc_s, True)
        else:
            receive(level, exc_t, exc_s, True)
    if len(strides) < 2:
        pool_product()

    for r in range(2):
        for h in range(heads):
            p = r * heads + h
            begin = start_log[r : r + 1, h : h + 1]
            late_max = exc_s[r, h : h + 1, :]
            late_fall = exc_s[r, heads + h : heads + h + 1, :]
            level = jnp.maximum(begin + late_fall, late_max)
            early = jnp.exp(begin + late_fall - level)
            late = jnp.exp(late_max - level)
            first = jnp.concatenate(
                [start_mem[r, h], jnp.broadcast_to(start_norm[r, h : h + 1, :], (AUG - DH, DH))], axis=0
            )
            state = early * first + late * exc_t[p]
            for n, b in enumerate(order[r]):
                enter_t[p, b] = jnp.concatenate(
                    [state[:DH], jnp.broadcast_to(state[DH : DH + 1], (DH, DH))], axis=0
                ).astype(BF16)
                enter_s[b, p : p + 1, :] = level
                if n + 1 < blocks:
                    state, level, _unused = advance(p, b, state, level)

    def finish(b, target, target_rows, target_cols):
        rows = rows_of(b)
        columns = acol_ref[rows, :]
        for h in range(heads):
            cols = slice(h * DH, (h + 1) * DH)
            queries = q_ref[rows, cols]
            hidden = jnp.zeros((size, DH), F32)
            for r in range(2):
                p = r * heads + h
                top = enter_s[b, p : p + 1, 0:1]
                peak = columns[:, p : p + 1]
                joint = jnp.maximum(peak, top)
                full = jnp.exp(peak - joint) * locals_ref[p, rows, :] + jnp.exp(
                    top - joint
                ) * lax.dot_general(
                    queries, enter_t[p, b], (((1,), (1,)), ((), ())), preferred_element_type=F32
                )
                hidden = hidden + full[:, :DH] / jnp.maximum(jnp.abs(full[:, DH:]), 1.0)
            centered = hidden - jnp.mean(hidden, axis=1, keepdims=True)
            variance = jnp.mean(centered * centered, axis=1, keepdims=True)
            gate = 1.0 / (1.0 + jnp.exp(-o_ref[rows, cols].astype(F32)))
            gain = hgain_ref[:, pl.ds(pl.multiple_of(group * mem_width + h * DH, DH), DH)]
            target[target_rows, target_cols(h)] = (
                centered * lax.rsqrt(variance + HEAD_EPS) * gain * gate
            ).astype(BF16)

    for other, copy in zip(others, mem_copies):
        finish(other, mem_out, rows_of(other), lambda h: slice(h * DH, (h + 1) * DH))
        copy.start()
    finish(
        group, lhs_mem, slice(None),
        lambda h: pl.ds(pl.multiple_of(group * mem_width + h * DH, DH), DH),
    )
    for copy in mem_copies:
        copy.wait_recv()
    tile = 512
    for n in range(out_ref.shape[1] // tile):
        cols = slice(n * tile, (n + 1) * tile)
        out_ref[:, cols] = (
            acc[:, cols] + jnp.dot(lhs_mem[...], wmo[:, cols], preferred_element_type=F32)
        ).astype(BF16)

    for c in range(blocks):
        to_far[c].wait_send()
        to_near[c].wait_send()
        onward[c].wait_send()
    for copy in pool_copies + mem_copies:
        copy.wait_send()
    for level in range(len(strides)):
        for r in range(2):
            okay, other, _unused = route(level, r)

            @pl.when(okay)
            def _():
                for copy in copies(level, r, other):
                    copy.wait_send()
    for side in range(2):
        @pl.when(rim_sends[side])
        def _():
            rim(side).wait_send()


def per_device(
    tokens,
    input_norm_gain,
    pooling_input_matrix,
    query_projection_matrix,
    key_projection_matrix,
    value_projection_matrix,
    output_gate_matrix,
    input_gate_matrix,
    forget_gate_matrix,
    forget_gate_bias,
    log_forget_scale,
    extra_log_forget,
    starting_memory,
    starting_normalizer,
    starting_log_scale,
    pooling_group_map,
    pooling_channel_scale,
    memory_head_gain,
    pooling_output_matrix,
    memory_output_matrix,
):
    rows, own_width = tokens.shape
    tp_size = lax.axis_size("tp")
    sp_size = lax.axis_size("sp")
    model_width = own_width * tp_size
    group_dim = pooling_input_matrix.shape[1]
    heads = query_projection_matrix.shape[1] // DH
    mem_width = heads * DH
    pairs = 2 * heads
    levels = max(1, (sp_size - 1).bit_length())
    blocks = tp_size
    size = rows // blocks
    all_heads = input_gate_matrix.shape[2]
    pool_total = pooling_output_matrix.shape[0]
    mem_total = memory_output_matrix.shape[0]
    anywhere = pl.BlockSpec(memory_space=pl.ANY)
    dma = pltpu.SemaphoreType.DMA
    return pl.pallas_call(
        functools.partial(layer_kernel, tp_size, sp_size, heads),
        out_shape=jax.ShapeDtypeStruct((size, model_width), BF16),
        in_specs=whole_vmem(13) + [anywhere] * 7,
        out_specs=pl.BlockSpec(memory_space=pltpu.VMEM),
        scratch_shapes=[
            VMEM((3, rows, own_width), BF16),
            VMEM((size, model_width), BF16),
            VMEM((4 * all_heads, model_width), BF16),
            VMEM((model_width, group_dim), BF16),
        ]
        + [VMEM((model_width, mem_width), BF16)] * 4
        + [
            VMEM((pool_total, model_width), BF16),
            VMEM((mem_total, model_width), BF16),
            VMEM((rows + 2 * RIM, group_dim), F32),
        ]
        + [VMEM((rows, mem_width), BF16)] * 4
        + [
            VMEM((4 * all_heads, size), F32),
            VMEM((pairs, blocks, AUG, DH), F32),
            VMEM((pairs, size), F32),
            VMEM((rows, 128), F32),
            VMEM((blocks, 2 * pairs, 128), F32),
            VMEM((pairs, rows, 2 * DH), F32),
            VMEM((pairs, AUG, DH), F32),
            VMEM((2, 2 * heads, 128), F32),
            VMEM((pairs, AUG, DH), F32),
            VMEM((2, 2 * heads, 128), F32),
            VMEM((levels, 2, heads, AUG, DH), BF16),
            VMEM((levels, 2, 2 * heads, 128), F32),
            VMEM((levels, 2, heads, AUG, DH), BF16),
            VMEM((levels, 2, 2 * heads, 128), F32),
            VMEM((2, RIM, group_dim), BF16),
            VMEM((2, RIM, group_dim), BF16),
            VMEM((pairs, blocks, 2 * DH, DH), BF16),
            VMEM((blocks, pairs, 128), F32),
            VMEM((rows, group_dim), BF16),
            VMEM((rows, mem_width), BF16),
            VMEM((size, pool_total), BF16),
            VMEM((size, mem_total), BF16),
            VMEM((size, model_width), F32),
        ]
        + [dma((7,))]
        + [dma((blocks,))] * 6
        + [dma((levels, 2))] * 4
        + [dma((2,))] * 2
        + [dma((3,))] * 4,
        compiler_params=pltpu.CompilerParams(
            collective_id=0, has_side_effects=True, vmem_limit_bytes=52 * 1024 * 1024
        ),
    )(
        tokens,
        input_norm_gain.reshape(1, model_width),
        input_gate_matrix.transpose(1, 2, 0),
        forget_gate_matrix.transpose(1, 2, 0),
        log_forget_scale,
        extra_log_forget,
        forget_gate_bias,
        starting_memory,
        starting_normalizer,
        starting_log_scale,
        pooling_group_map,
        pooling_channel_scale.reshape(1, pool_total),
        memory_head_gain.reshape(1, mem_total),
        pooling_input_matrix,
        query_projection_matrix,
        key_projection_matrix,
        value_projection_matrix,
        output_gate_matrix,
        pooling_output_matrix,
        memory_output_matrix,
    )


def solution(mesh):
    placed = (
        P("sp", "tp"),
        P(),
        P(None, "tp"),
        P(None, "tp"),
        P(None, "tp"),
        P(None, "tp"),
        P(None, "tp"),
        P(),
        P(),
        P(),
        P(None, "sp"),
        P(None, "sp"),
        P(None, "tp", None, None),
        P(None, "tp", None),
        P(None, "tp"),
        P(),
        P(),
        P(),
        P(),
        P(),
    )
    return jax.shard_map(
        per_device, mesh=mesh, in_specs=placed, out_specs=P(("sp", "tp"), None), check_vma=False
    )
```
